32 devices in a mesh: sp: 8 (over z, x), tp: 4 (over y, core).
Axes of the slice: x: 2, y: 2, z: 4, core: 2. Of those that a mesh axis runs over, the one named last changes fastest.
Arguments:
- token_grid: bfloat16 [8, 2048, 512], P('sp', 'tp'), may hold values from -6 to 6
- norm_gain: bfloat16 [3, 2048], replicated, may hold values from 0.099609375 to 1.8984375
- w_query: bfloat16 [3, 2048, 2048], P(None, None, 'tp'), may hold values from -0.125 to 0.125
- w_key: bfloat16 [3, 2048, 2048], P(None, None, 'tp'), may hold values from -0.125 to 0.125
- w_value: bfloat16 [3, 2048, 2048], P(None, None, 'tp'), may hold values from -0.125 to 0.125
- w_out: bfloat16 [3, 2048, 2048], P(None, 'tp'), may hold values from -0.5 to 0.5
- rel_bias: float32 [3, 32, 8, 16], P(None, 'tp'), may hold values from -3 to 250
Outputs:
- grid_out: bfloat16 [8, 2048, 512], P('sp', 'tp')
The draws below stay inside these ranges and needn't reach their ends.
All inputs are finite; a program needn't handle non-finite values.
Results may differ from the reference program's by a relative error of at most 0.024.
Values may be sent and summed in bfloat16 or wider, within the bound.
No kernel may reach another device: no remote copies, remote signals or barrier semaphores. Data moves between devices by JAX's collectives and lax.ppermute only.
A program may use at most 128 MiB of HBM per device.

```python
import jax
import jax.numpy as jnp
from jax import lax

D = 2048
HEADS = 32
HEAD_DIM = 64
WIN_R = 8
WIN_C = 16
LAYERS = 3
COLS = 512
ROWS = 8
N_TP = 4


def draw_rel_bias(key, part):
    dims_all = (LAYERS, HEADS, WIN_R, WIN_C)
    baseline = jnp.clip(jax.random.normal(jax.random.fold_in(key, 11), dims_all, jnp.float32), -3.0, 3.0)
    return baseline


def block_scale(own_key, shape, shards, low, high):
    def one(axis_at, shards_of):
        steps = jax.random.uniform(jax.random.fold_in(jax.random.fold_in(own_key, 6), axis_at), (shards_of,), jnp.float32, low / len(shards), high / len(shards))
        return jnp.repeat(jnp.exp(steps), shape[axis_at] // shards_of).reshape((-1,) + (1,) * (len(shape) - axis_at - 1))

    factor_of = one(*shards[0])
    for cut in shards[1:]:
        factor_of = factor_of * one(*cut)
    return factor_of


def scatter_about(key, dims, deviation, most, pieces=(), kind=jnp.bfloat16):
    drawn = deviation * jax.random.normal(key, dims, jnp.float32)
    if pieces:
        drawn = drawn * block_scale(key, dims, pieces, -0.22, 0.18)
    return jnp.clip(drawn, -most, most).astype(kind)


def setup_inputs(seed: int = 0) -> dict:
    keys = jax.random.split(jax.random.key(seed), 8)
    return {
        "token_grid": scatter_about(keys[0], (ROWS, D, COLS), 1.0, 6.0, ((0, 8), (1, 4))),
        "norm_gain": jnp.clip(1.0 + 0.18 * jax.random.normal(keys[1], (LAYERS, D), jnp.float32), 0.099609375, 1.8984375).astype(jnp.bfloat16),
        "w_query": scatter_about(keys[2], (LAYERS, D, D), D ** -0.5, 0.125, ((2, 4),)),
        "w_key": scatter_about(keys[3], (LAYERS, D, D), D ** -0.5, 0.125, ((2, 4),)),
        "w_value": scatter_about(keys[4], (LAYERS, D, D), D ** -0.5, 0.125, ((2, 4),)),
        "w_out": scatter_about(keys[5], (LAYERS, D, D), (D // 16) ** -0.5, 0.5, ((1, 4),)),
        "rel_bias": draw_rel_bias(jax.random.fold_in(keys[7], 71), 0),
    }


EPS = 1e-06

def rounded(source):
    return lax.optimization_barrier(source.astype(jnp.bfloat16)).astype(jnp.float32)

def one_layer(token_grid, gain_row, w_query, w_key, w_value, w_out, bias_table):
    grid_wide = token_grid.astype(jnp.float32)
    inverse = lax.rsqrt(lax.optimization_barrier(jnp.mean(grid_wide * grid_wide, axis=1)) + EPS)
    scaled = (grid_wide * gain_row.astype(jnp.float32)[None, :, None]).astype(jnp.bfloat16)
    flat_rows = jnp.transpose(scaled, (0, 2, 1)).reshape(ROWS * COLS, D)
    inverse_flat = inverse.reshape(ROWS * COLS, 1)

    def project(weight):
        product = jnp.dot(flat_rows, weight, preferred_element_type=jnp.float32) * inverse_flat
        return rounded(product).reshape(ROWS, COLS, HEADS, HEAD_DIM)
    queries = project(w_query)
    keys_all = project(w_key)
    values_all = project(w_value)
    factor = HEAD_DIM ** (-0.5)
    offsets = jnp.arange(WIN_R * WIN_C, dtype=jnp.int32)

    def scores_at(offset):
        slot_row = offset // WIN_C
        slot_col = offset % WIN_C
        rolled = jnp.roll(keys_all, (WIN_R // 2 - slot_row, WIN_C // 2 - slot_col), axis=(0, 1))
        offset_bias = lax.dynamic_slice(bias_table, (jnp.int32(0), slot_row, slot_col), (HEADS, 1, 1)).reshape(HEADS)
        return lax.optimization_barrier(jnp.sum(queries * rolled, axis=-1)) * factor + offset_bias
    scores = lax.map(scores_at, offsets)
    weights = rounded(jax.nn.softmax(scores, axis=0))

    def accumulate(running, operands):
        weight_now, offset = operands
        slot_row = offset // WIN_C
        slot_col = offset % WIN_C
        rolled = jnp.roll(values_all, (WIN_R // 2 - slot_row, WIN_C // 2 - slot_col), axis=(0, 1))
        return (running + weight_now[..., None] * rolled, None)
    mixed_out, unused = lax.scan(accumulate, jnp.zeros((ROWS, COLS, HEADS, HEAD_DIM), jnp.float32), (weights, offsets))
    mixed_out = mixed_out.astype(jnp.bfloat16).reshape(ROWS * COLS, N_TP, D // N_TP)
    groups = jnp.moveaxis(mixed_out, 1, 0)
    blocks = w_out.reshape(N_TP, D // N_TP, D)

    def add_group(running, operands):
        partial_value = jnp.dot(operands[0], operands[1], preferred_element_type=jnp.float32)
        return (running + rounded(partial_value), None)
    update, unused = lax.scan(add_group, jnp.zeros((ROWS * COLS, D), jnp.float32), (groups, blocks))
    update = jnp.transpose(update.reshape(ROWS, COLS, D), (0, 2, 1))
    return (grid_wide + update).astype(jnp.bfloat16)

def reference(token_grid, norm_gain, w_query, w_key, w_value, w_out, rel_bias):
    current = token_grid
    for layer_idx in range(LAYERS):
        current = one_layer(current, norm_gain[layer_idx], w_query[layer_idx], w_key[layer_idx], w_value[layer_idx], w_out[layer_idx], rel_bias[layer_idx])
    return current
```

```python
import functools
import math

import jax
import jax.numpy as jnp
from jax import lax
from jax.experimental import pallas as pl
from jax.experimental.pallas import tpu as pltpu
from jax.sharding import PartitionSpec as P

HEAD_DIM = 64
WIN_R = 8
WIN_C = 16
HALF_R = WIN_R // 2
HALF_C = WIN_C // 2
EPS = 1e-06
LOG2E = math.log2(math.e)
Q_SCALE = HEAD_DIM ** (-0.5) * LOG2E
MASKED = -1e30
BLOCK = 128
F32 = jnp.float32
BF16 = jnp.bfloat16


def _permute_kernel(x_ref, o_ref, *, rows, cols):
    tokens = rows * cols
    out_at = lax.broadcasted_iota(jnp.int32, (tokens, tokens), 0)
    in_at = lax.broadcasted_iota(jnp.int32, (tokens, tokens), 1)
    pick = (out_at % rows) * cols + out_at // rows == in_at
    o_ref[...] = jnp.dot(
        pick.astype(F32).astype(BF16), x_ref[...], preferred_element_type=F32
    ).astype(BF16)


def permute_tokens(x, rows, cols):
    return pl.pallas_call(
        functools.partial(_permute_kernel, rows=rows, cols=cols),
        out_shape=jax.ShapeDtypeStruct(x.shape, BF16),
        name="to_column_order",
    )(x)


def _qkv_kernel(ids_ref, *refs, n_parts, halo, d_model):
    parts = refs[:n_parts]
    gain_ref, wq_ref, wk_ref, wv_ref = refs[n_parts : n_parts + 4]
    q_ref, k_ref, v_ref, first_ref, last_ref = refs[n_parts + 4 : n_parts + 9]
    scaled_ref, inverse_ref = refs[n_parts + 9 :]
    tokens, chunk = parts[0].shape

    @pl.when(pl.program_id(0) == 0)
    def _():
        squares = jnp.zeros((tokens, 128), F32)
        for at, part in enumerate(parts):
            wide = part[...].astype(F32)
            where = ids_ref[at]
            scaled_ref[where] = (wide * gain_ref[0, where]).astype(BF16)
            for lane in range(0, chunk, 128):
                tile = wide[:, lane : lane + 128]
                squares = squares + tile * tile
        total = jnp.sum(squares, axis=1, keepdims=True)
        inverse_ref[...] = lax.rsqrt(total / d_model + EPS)

    scaled = jnp.concatenate([scaled_ref[at] for at in range(n_parts)], axis=1)
    inverse = inverse_ref[...]
    k = (jnp.dot(scaled, wk_ref[0], preferred_element_type=F32) * inverse).astype(BF16)
    k_ref[...] = k
    v = (jnp.dot(scaled, wv_ref[0], preferred_element_type=F32) * inverse).astype(BF16)
    v_ref[...] = v
    first_ref[0] = k[:halo]
    first_ref[1] = v[:halo]
    last_ref[0] = k[tokens - halo :]
    last_ref[1] = v[tokens - halo :]
    q = jnp.dot(scaled, wq_ref[0], preferred_element_type=F32) * (inverse * Q_SCALE)
    q_ref[...] = q.astype(BF16)


def qkv(layer, parts, ids, gains, w_query, w_key, w_value, halo):
    tokens, chunk = parts[0].shape
    n_parts = len(parts)
    d_model = n_parts * chunk
    channels = w_query.shape[2]
    tile = min(256, channels)
    whole = pl.BlockSpec((tokens, chunk), lambda j, ids: (0, 0))
    weight = pl.BlockSpec((1, d_model, tile), lambda j, ids: (layer, 0, j))
    out_tile = pl.BlockSpec((tokens, tile), lambda j, ids: (0, j))
    edge = pl.BlockSpec((2, halo, tile), lambda j, ids: (0, 0, j))
    out = jax.ShapeDtypeStruct((tokens, channels), BF16)
    edge_out = jax.ShapeDtypeStruct((2, halo, channels), BF16)
    return pl.pallas_call(
        functools.partial(_qkv_kernel, n_parts=n_parts, halo=halo, d_model=d_model),
        grid_spec=pltpu.PrefetchScalarGridSpec(
            num_scalar_prefetch=1,
            grid=(channels // tile,),
            in_specs=[whole] * n_parts
            + [pl.BlockSpec((1, n_parts, 1, chunk), lambda j, ids: (layer, 0, 0, 0))]
            + [weight] * 3,
            out_specs=[out_tile] * 3 + [edge] * 2,
            scratch_shapes=[
                pltpu.VMEM((n_parts, tokens, chunk), BF16),
                pltpu.VMEM((tokens, 1), F32),
            ],
        ),
        out_shape=[out] * 3 + [edge_out] * 2,
        name="qkv",
    )(ids, *parts, gains, w_query, w_key, w_value)


def _attention_kernel(
    q_ref, k_ref, v_ref, before_ref, after_ref, base_ref, o_ref, k_all, v_all, bias_ref, *, rows
):
    tokens = q_ref.shape[0]
    halo = before_ref.shape[1]
    window = base_ref.shape[3]
    k_all[:halo] = before_ref[0]
    v_all[:halo] = before_ref[1]
    k_all[halo : halo + tokens] = k_ref[...]
    v_all[halo : halo + tokens] = v_ref[...]
    k_all[halo + tokens :] = after_ref[0]
    v_all[halo + tokens :] = after_ref[1]
    for head in range(2):
        base = base_ref[0, head]
        for col in range(BLOCK // rows):
            shifted = base if col == 0 else pltpu.roll(base, col * rows, 1)
            bias_ref[head * BLOCK + col * rows : head * BLOCK + (col + 1) * rows] = shifted
    low = lax.broadcasted_iota(jnp.int32, (BLOCK, 2 * HEAD_DIM), 1) < HEAD_DIM
    ones = jnp.ones((window, 2 * HEAD_DIM), BF16)
    for at in range(0, tokens, BLOCK):
        q = q_ref[at : at + BLOCK].astype(F32)
        both = jnp.concatenate([jnp.where(low, q, 0.0), jnp.where(low, 0.0, q)], axis=0)
        keys = k_all[at : at + window]
        scores = lax.dot_general(
            both.astype(BF16), keys, (((1,), (1,)), ((), ())), preferred_element_type=F32
        )
        scores = scores + bias_ref[...]
        highest = jnp.max(scores, axis=1, keepdims=True)
        weights = jnp.exp2(scores - highest).astype(BF16)
        values = jnp.concatenate([v_all[at : at + window], ones], axis=1)
        mixed = jnp.dot(weights, values, preferred_element_type=F32)
        width = 2 * HEAD_DIM
        top = jnp.where(low, mixed[:BLOCK, :width], mixed[BLOCK:, :width])
        total = jnp.where(low, mixed[:BLOCK, width:], mixed[BLOCK:, width:])
        o_ref[at : at + BLOCK] = (top / total).astype(BF16)


def attention(layer, q, k, v, before, after, bases, rows):
    tokens, channels = q.shape
    halo = before.shape[1]
    window = bases.shape[3]
    width = 2 * HEAD_DIM
    pair = pl.BlockSpec((tokens, width), lambda p: (0, p))
    edge = pl.BlockSpec((2, halo, width), lambda p: (0, 0, p))
    return pl.pallas_call(
        functools.partial(_attention_kernel, rows=rows),
        grid=(channels // width,),
        in_specs=[pair] * 3
        + [edge] * 2
        + [pl.BlockSpec((1, 2, rows, window), lambda p: (layer, p, 0, 0))],
        out_specs=pair,
        scratch_shapes=[
            pltpu.VMEM((tokens + 2 * halo, width), BF16),
            pltpu.VMEM((tokens + 2 * halo, width), BF16),
            pltpu.VMEM((2 * BLOCK, window), F32),
        ],
        out_shape=jax.ShapeDtypeStruct((tokens, channels), BF16),
        name="attention",
    )(q, k, v, before, after, bases)


def _project_kernel(id_ref, own_ref, other_ref, w_own_ref, w_other_ref, o_ref):
    acc = jnp.dot(own_ref[...], w_own_ref[0], preferred_element_type=F32)
    acc = acc + jnp.dot(other_ref[...], w_other_ref[0], preferred_element_type=F32)
    o_ref[...] = acc.astype(BF16)


def project(layer, own, other, w_out, w_other, chunk_id):
    tokens, channels = own.shape
    chunk = w_other.shape[2]
    tile = min(256, chunk)
    steps = chunk // tile
    mixed = pl.BlockSpec((tokens, channels), lambda j, at: (0, 0))
    return pl.pallas_call(
        _project_kernel,
        grid_spec=pltpu.PrefetchScalarGridSpec(
            num_scalar_prefetch=1,
            grid=(steps,),
            in_specs=[
                mixed,
                mixed,
                pl.BlockSpec((1, channels, tile), lambda j, at: (layer, 0, at[0] * steps + j)),
                pl.BlockSpec((1, channels, tile), lambda j, at: (layer, 0, j)),
            ],
            out_specs=pl.BlockSpec((tokens, tile), lambda j, at: (0, j)),
        ),
        out_shape=jax.ShapeDtypeStruct((tokens, chunk), BF16),
        name="project",
    )(chunk_id, own, other, w_out, w_other)


def _finish_kernel(x_ref, *refs, rows, cols):
    o_ref = refs[-1]
    tokens = rows * cols
    update = refs[0][...].astype(F32)
    for ref in refs[1:-1]:
        update = update + ref[...].astype(F32)
    grid = (x_ref[...].astype(F32) + update).astype(BF16)
    out_at = lax.broadcasted_iota(jnp.int32, (tokens, tokens), 0)
    in_at = lax.broadcasted_iota(jnp.int32, (tokens, tokens), 1)
    pick = (out_at % cols) * rows + out_at // cols == in_at
    o_ref[...] = jnp.dot(
        pick.astype(F32).astype(BF16), grid, preferred_element_type=F32
    ).astype(BF16)


def finish(x, partials, rows, cols):
    return pl.pallas_call(
        functools.partial(_finish_kernel, rows=rows, cols=cols),
        out_shape=jax.ShapeDtypeStruct(x.shape, BF16),
        name="to_row_order",
    )(x, *partials)


def ring_order(mesh):
    n_sp = mesh.shape["sp"]
    at = list(mesh.axis_names).index("sp")
    devices = mesh.devices if at == 0 else mesh.devices.T
    try:
        places = [tuple(devices[i].flat[0].coords) for i in range(n_sp)]
    except Exception:
        return list(range(n_sp))
    xs = sorted({p[0] for p in places})
    zs = sorted({p[2] for p in places})
    index = {(p[0], p[2]): i for i, p in enumerate(places)}
    if len(index) != n_sp or len(xs) * len(zs) != n_sp:
        return list(range(n_sp))
    path = [(xs[0], z) for z in zs]
    for turn, z in enumerate(reversed(zs)):
        line = xs[1:] if turn % 2 == 0 else xs[1:][::-1]
        path += [(x, z) for x in line]
    return [index[p] for p in path]


def dense_bias(rel_bias, rows, window):
    layers, heads = rel_bias.shape[:2]
    span = WIN_C * rows
    slot = lax.broadcasted_iota(jnp.int32, (WIN_R * WIN_C, rows * span), 0)
    place = lax.broadcasted_iota(jnp.int32, (WIN_R * WIN_C, rows * span), 1)
    row_slot = (place % rows - place // span + HALF_R) % rows
    col_slot = (place % span) // rows
    pick = (slot // WIN_C == row_slot) & (slot % WIN_C == col_slot)
    flat = rel_bias.reshape(layers * heads, WIN_R * WIN_C) * LOG2E
    base = jnp.dot(flat, pick.astype(F32), precision=lax.Precision.HIGHEST)
    base = jnp.where(row_slot[:1] < WIN_R, base, MASKED)
    base = base.reshape(layers, heads, rows, span)
    return jnp.pad(base, ((0, 0),) * 3 + ((0, window - span),), constant_values=MASKED)


def body(
    token_grid, norm_gain, w_query, w_key, w_value, w_out, rel_bias, *, order
):
    n_sp = lax.axis_size("sp")
    n_tp = lax.axis_size("tp")
    n_y = n_tp // 2
    layers = norm_gain.shape[0]
    chunk = token_grid.shape[1]
    rows = n_sp * token_grid.shape[0]
    cols = token_grid.shape[2] // n_sp
    tokens = rows * cols
    halo = HALF_C * rows
    window = BLOCK + 2 * halo
    here = lax.axis_index("tp")
    my_y, my_core = here // 2, here % 2
    rank = [order.index(i) for i in range(n_sp)]
    after_of = [(order[i], order[(i + 1) % n_sp]) for i in range(n_sp)]
    before_of = [(b, a) for a, b in after_of]

    def over_core(x):
        return lax.ppermute(x, "tp", [(i, i ^ 1) for i in range(n_tp)])

    def over_y(x, shift):
        return lax.ppermute(x, "tp", [(i, (i + 2 * shift) % n_tp) for i in range(n_tp)])

    blocks = token_grid[0].T.reshape(n_sp, cols, chunk)
    blocks = jnp.stack([blocks[rank[i]] for i in range(n_sp)])
    mine = lax.all_to_all(blocks, "sp", 0, 0, tiled=True).reshape(tokens, chunk)
    mine = permute_tokens(mine, rows, cols)

    w_others = []
    for y in range(n_y):
        theirs = lax.dynamic_slice_in_dim(w_out, (2 * y + 1 - my_core) * chunk, chunk, 2)
        w_others.append(over_core(theirs))
    gains = norm_gain.astype(F32).reshape(layers, n_tp, 1, chunk)
    bases = dense_bias(rel_bias, rows, window)

    own = [mine] + [over_y(mine, shift) for shift in range(1, n_y)]
    ys = [(my_y - shift) % n_y for shift in range(n_y)]
    grids = own
    for layer in range(layers):
        other = [over_core(x) for x in grids]
        ids = jnp.stack([2 * y + my_core for y in ys] + [2 * y + 1 - my_core for y in ys])
        q, k, v, first, last = qkv(
            layer, grids + other, ids.astype(jnp.int32), gains, w_query, w_key, w_value, halo
        )
        after = lax.ppermute(first, "sp", before_of)
        before = lax.ppermute(last, "sp", after_of)
        mixed = attention(layer, q, k, v, before, after, bases, rows)
        mixed_other = over_core(mixed)

        def partial_of(y, w_other):
            chunk_id = (2 * y + my_core).astype(jnp.int32).reshape(1)
            return project(layer, mixed, mixed_other, w_out, w_other, chunk_id)

        if layer == 0:
            absolute = []
            for y in range(n_y):
                pick = own[0]
                for shift in range(1, n_y):
                    pick = jnp.where(ys[shift] == y, own[shift], pick)
                absolute.append(pick)
            grids = absolute
            ys = [jnp.int32(y) for y in range(n_y)]
        if layer + 1 < layers:
            fresh = []
            for y in range(n_y):
                partial = partial_of(jnp.int32(y), w_others[y])
                update = partial.astype(F32)
                for shift in range(1, n_y):
                    update = update + over_y(partial, shift).astype(F32)
                fresh.append((grids[y].astype(F32) + update).astype(BF16))
            grids = fresh
        else:
            def select(arrays, y):
                pick = arrays[0]
                for at in range(1, n_y):
                    pick = jnp.where(y == at, arrays[at], pick)
                return pick

            partials = []
            for shift in list(range(1, n_y)) + [0]:
                y = (my_y + shift) % n_y
                partial = partial_of(y, select(w_others, y))
                partials.append(partial if shift == 0 else over_y(partial, shift))
            done = finish(select(grids, my_y), partials[::-1], rows, cols)

    sent = lax.all_to_all(done.reshape(n_sp, cols, chunk), "sp", 0, 0, tiled=True)
    sent = jnp.stack([sent[order[i]] for i in range(n_sp)])
    return sent.reshape(n_sp * cols, chunk).T[None]


def solution(mesh):
    in_specs = (
        P("sp", "tp", None),
        P(),
        P(None, None, "tp"),
        P(None, None, "tp"),
        P(None, None, "tp"),
        P(None, "tp", None),
        P(None, "tp", None, None),
    )
    out_specs = P("sp", "tp", None)
    return jax.shard_map(
        functools.partial(body, order=ring_order(mesh)),
        mesh=mesh,
        in_specs=in_specs,
        out_specs=out_specs,
        check_vma=False,
    )
```

```python
import functools
import math

import jax
import jax.numpy as jnp
from jax import lax
from jax.experimental import pallas as pl
from jax.experimental.pallas import tpu as pltpu
from jax.sharding import PartitionSpec as P

HEAD_DIM = 64
WIN_R = 8
WIN_C = 16
HALF_R = WIN_R // 2
HALF_C = WIN_C // 2
EPS = 1e-06
LOG2E = math.log2(math.e)
Q_SCALE = HEAD_DIM ** (-0.5) * LOG2E
MASKED = -1e30
BLOCK = 128
F32 = jnp.float32
BF16 = jnp.bfloat16
VMEM_LIMIT = 14 * 1024 * 1024
NT = (((1,), (1,)), ((), ()))
TN = (((0,), (0,)), ((), ()))


def call(kernel, name, outs, *args, scalars=(), scratch=()):
    vmem = pl.BlockSpec(memory_space=pltpu.VMEM)
    smem = pl.BlockSpec(memory_space=pltpu.SMEM)
    return pl.pallas_call(
        kernel,
        in_specs=[smem] * len(scalars) + [vmem] * len(args),
        out_specs=[vmem] * len(outs),
        out_shape=[jax.ShapeDtypeStruct(shape, dtype) for shape, dtype in outs],
        scratch_shapes=list(scratch),
        compiler_params=pltpu.CompilerParams(vmem_limit_bytes=VMEM_LIMIT),
        name=name,
    )(*scalars, *args)


def one_hot(pick):
    return pick.astype(F32).astype(BF16)


def split_columns(x, picks, n_sp):
    chunk, columns = x.shape

    def kernel(x_ref, *outs):
        for out, (cols_of, rank) in zip(outs, picks):
            width = len(cols_of)
            at = lax.broadcasted_iota(jnp.int32, (width, columns), 0)
            source = lax.broadcasted_iota(jnp.int32, (width, columns), 1)
            local = part_column(at, cols_of)
            for device in range(n_sp):
                first = rank[device] * (columns // n_sp)
                out[device] = lax.dot_general(
                    one_hot(source == local + first), x_ref[...], NT, preferred_element_type=F32
                ).astype(BF16)

    outs = [((n_sp, len(cols_of), chunk), BF16) for cols_of, _ in picks]
    return call(kernel, "split_columns", outs, x)


def part_column(at, cols_of):
    jump = next((i for i in range(1, len(cols_of)) if cols_of[i] != cols_of[i - 1] + 1), None)
    local = at + cols_of[0]
    if jump is not None:
        local = local + jnp.where(at >= jump, cols_of[jump] - cols_of[0] - jump, 0)
    return local


def merge_columns(parts, picks, columns, n_sp):
    chunk = parts[0].shape[2]
    per = columns // n_sp

    def kernel(*refs):
        out = refs[-1]
        acc = jnp.zeros((chunk, columns), F32)
        for ref, (cols_of, rank) in zip(refs, picks):
            width = len(cols_of)
            at = lax.broadcasted_iota(jnp.int32, (width, columns), 0)
            target = lax.broadcasted_iota(jnp.int32, (width, columns), 1)
            local = part_column(at, cols_of)
            pick = jnp.concatenate(
                [one_hot(target == local + rank[device] * per) for device in range(n_sp)], axis=0
            )
            rows = jnp.concatenate([ref[device] for device in range(n_sp)], axis=0)
            acc = acc + lax.dot_general(rows, pick, TN, preferred_element_type=F32)
        out[...] = acc.astype(BF16)

    return call(kernel, "merge_columns", [((chunk, columns), BF16)], *parts)[0]


def to_column_order(x):
    rows, cols, chunk = x.shape
    tokens = rows * cols

    def kernel(x_ref, o_ref):
        out_at = lax.broadcasted_iota(jnp.int32, (tokens, tokens), 0)
        in_at = lax.broadcasted_iota(jnp.int32, (tokens, tokens), 1)
        pick = one_hot((out_at % rows) * cols + out_at // rows == in_at)
        source = jnp.concatenate([x_ref[row] for row in range(rows)], axis=0)
        o_ref[...] = jnp.dot(pick, source, preferred_element_type=F32).astype(BF16)

    return call(kernel, "to_column_order", [((tokens, chunk), BF16)], x)[0]


def expand_bias(bases, rows):
    tables, _, window = bases.shape

    def kernel(base_ref, o_ref):
        def one(table, carry):
            base = base_ref[table]
            for col in range(BLOCK // rows):
                shifted = base if col == 0 else pltpu.roll(base, col * rows, 1)
                o_ref[table, col * rows : (col + 1) * rows] = shifted
            return carry

        lax.fori_loop(0, tables, one, 0)

    return call(kernel, "expand_bias", [((tables, BLOCK, window), F32)], bases)[0]


def qkv(layer, parts, ids, gains, w_query, w_key, w_value, halo):
    tokens = parts[0].shape[0]
    chunk = gains.shape[3]
    n_tp = gains.shape[1]
    d_model = n_tp * chunk
    channels = w_query.shape[2]
    pieces = [(i, lo) for i, part in enumerate(parts) for lo in range(0, part.shape[1], chunk)]

    def kernel(ids_ref, *refs):
        ins = refs[: len(parts)]
        gain_ref, wq_ref, wk_ref, wv_ref = refs[len(parts) : len(parts) + 4]
        outs = refs[len(parts) + 4 : -1]
        scaled_ref = refs[-1]
        squares = jnp.zeros((tokens, 128), F32)
        for at, (i, lo) in enumerate(pieces):
            wide = ins[i][:, lo : lo + chunk].astype(F32)
            where = ids_ref[at]
            scaled_ref[where] = (wide * gain_ref[layer, where]).astype(BF16)
            for lane in range(0, chunk, 128):
                tile = wide[:, lane : lane + 128]
                squares = squares + tile * tile
        inverse = lax.rsqrt(jnp.sum(squares, axis=1, keepdims=True) / d_model + EPS)
        scaled = jnp.concatenate([scaled_ref[at] for at in range(n_tp)], axis=1)

        def times(w_ref, scale):
            return (jnp.dot(scaled, w_ref[layer], preferred_element_type=F32) * scale).astype(BF16)

        for at, w_ref in ((1, wk_ref), (2, wv_ref)):
            out = times(w_ref, inverse)
            outs[at][...] = out
            if halo:
                outs[3][at - 1] = out[:halo]
                outs[4][at - 1] = out[tokens - halo :]
        outs[0][...] = times(wq_ref, inverse * Q_SCALE)

    outs = [((tokens, channels), BF16)] * 3
    if halo:
        outs += [((2, halo, channels), BF16)] * 2
    return call(
        kernel,
        "qkv",
        outs,
        *parts,
        gains,
        w_query,
        w_key,
        w_value,
        scalars=(ids,),
        scratch=[pltpu.VMEM((n_tp, tokens, chunk), BF16)],
    )


def attention(layer, starts, q, sources, segments, bias):
    tokens, channels = q.shape
    window = bias.shape[2]
    halo = (window - BLOCK) // 2
    width = 2 * HEAD_DIM
    heads = channels // HEAD_DIM

    def kernel(q_ref, *refs):
        bias_ref, o_ref = refs[-2:]

        def read(of_value, low, lanes):
            pieces = []
            for first, rows, source, row in segments:
                lo, hi = max(low, first), min(low + window, first + rows)
                if lo >= hi:
                    continue
                at = slice(row + lo - first, row + hi - first)
                if isinstance(source, tuple):
                    pieces.append(refs[source[of_value]][at, lanes])
                else:
                    pieces.append(refs[source][of_value, at, lanes])
            return jnp.concatenate(pieces, axis=0)

        low_half = lax.broadcasted_iota(jnp.int32, (BLOCK, width), 1) < HEAD_DIM
        ones = jnp.ones((window, width), BF16)

        def one_pair(pair, carry):
            lanes = pl.ds(pl.multiple_of(pair * width, width), width)
            for at, start in enumerate(starts):
                rows = slice(at * BLOCK, (at + 1) * BLOCK)
                q_wide = q_ref[rows, lanes].astype(F32)
                both = jnp.concatenate(
                    [jnp.where(low_half, q_wide, 0.0), jnp.where(low_half, 0.0, q_wide)], axis=0
                )
                scores = lax.dot_general(
                    both.astype(BF16),
                    read(0, start - halo, lanes),
                    NT,
                    preferred_element_type=F32,
                )
                table = layer * heads + 2 * pair
                scores = scores + jnp.concatenate([bias_ref[table], bias_ref[table + 1]], axis=0)
                highest = jnp.max(scores, axis=1, keepdims=True)
                weights = jnp.exp2(scores - highest).astype(BF16)
                values = jnp.concatenate([read(1, start - halo, lanes), ones], axis=1)
                mixed = jnp.dot(weights, values, preferred_element_type=F32)
                top = jnp.where(low_half, mixed[:BLOCK, :width], mixed[BLOCK:, :width])
                total = jnp.where(low_half, mixed[:BLOCK, width:], mixed[BLOCK:, width:])
                o_ref[rows, lanes] = (top / total).astype(BF16)
            return carry

        lax.fori_loop(0, channels // width, one_pair, 0)

    return call(kernel, "attention", [((tokens, channels), BF16)], q, *sources, bias)[0]


def project(layer, own, other, w_out, w_other, ys, my_core, joined):
    tokens, channels = own.shape
    chunk = w_other.shape[3]
    count = ys.shape[0]

    def kernel(ys_ref, core_ref, own_ref, other_ref, w_out_ref, w_other_ref, *outs):
        for at in range(count):
            y = ys_ref[at]
            column = pl.multiple_of((2 * y + core_ref[0]) * chunk, chunk)
            acc = jnp.dot(
                own_ref[...], w_out_ref[layer, :, pl.ds(column, chunk)], preferred_element_type=F32
            )
            acc = acc + jnp.dot(other_ref[...], w_other_ref[y, layer], preferred_element_type=F32)
            if joined:
                outs[0][:, at * chunk : (at + 1) * chunk] = acc.astype(BF16)
            else:
                outs[at][...] = acc.astype(BF16)

    if joined:
        outs = [((tokens, count * chunk), BF16)]
    else:
        outs = [((tokens, chunk), BF16)] * count
    return call(
        kernel, "project", outs, own, other, w_out, w_other, scalars=(ys, my_core.reshape(1))
    )


def add_update(olds, partials, orders):
    tokens, wide = partials[0].shape
    chunk = wide // (wide // olds[0].shape[1]) if len(olds) > 1 else wide

    def kernel(where_ref, *refs):
        old_refs, partial_refs, o_ref = refs[: len(olds)], refs[len(olds) : -1], refs[-1]
        for at, lo in enumerate(range(0, wide, chunk)):
            old = old_refs[0][...].astype(F32)
            for piece in range(1, len(olds)):
                fresh = old_refs[piece][...].astype(F32)
                old = jnp.where(where_ref[at] == piece, fresh, old)
            update = partial_refs[0][:, lo : lo + chunk].astype(F32)
            for ref in partial_refs[1:]:
                update = update + ref[:, lo : lo + chunk].astype(F32)
            o_ref[:, lo : lo + chunk] = (old + update).astype(BF16)

    return call(
        kernel, "add_update", [((tokens, wide), BF16)], *olds, *partials, scalars=(orders,)
    )[0]


def finish(old, partials, my_y, rows, cols):
    tokens, chunk = partials[0].shape

    def kernel(y_ref, old_ref, *refs):
        o_ref = refs[-1]
        grid = old_ref[:, :chunk].astype(F32)
        for y in range(1, old.shape[1] // chunk):
            grid = jnp.where(y_ref[0] == y, old_ref[:, y * chunk : (y + 1) * chunk].astype(F32), grid)
        update = refs[0][...].astype(F32)
        for ref in refs[1:-1]:
            update = update + ref[...].astype(F32)
        grid = (grid + update).astype(BF16)
        out_at = lax.broadcasted_iota(jnp.int32, (tokens, tokens), 0)
        in_at = lax.broadcasted_iota(jnp.int32, (tokens, tokens), 1)
        pick = one_hot((out_at % cols) * rows + out_at // cols == in_at)
        moved = jnp.dot(pick, grid, preferred_element_type=F32).astype(BF16)
        for row in range(rows):
            o_ref[row] = moved[row * cols : (row + 1) * cols]

    return call(
        kernel, "finish", [((rows, cols, chunk), BF16)], old, *partials, scalars=(my_y.reshape(1),)
    )[0]


def ring_order(mesh):
    n_sp = mesh.shape["sp"]
    at = list(mesh.axis_names).index("sp")
    devices = mesh.devices if at == 0 else mesh.devices.T
    try:
        places = [tuple(devices[i].flat[0].coords) for i in range(n_sp)]
    except Exception:
        return list(range(n_sp))
    xs = sorted({p[0] for p in places})
    zs = sorted({p[2] for p in places})
    index = {(p[0], p[2]): i for i, p in enumerate(places)}
    if len(index) != n_sp or len(xs) * len(zs) != n_sp:
        return list(range(n_sp))
    path = [(xs[0], z) for z in zs]
    for turn, z in enumerate(reversed(zs)):
        line = xs[1:] if turn % 2 == 0 else xs[1:][::-1]
        path += [(x, z) for x in line]
    return [index[p] for p in path]


def dense_bias(rel_bias, rows, window):
    layers, heads = rel_bias.shape[:2]
    span = WIN_C * rows
    slot = lax.broadcasted_iota(jnp.int32, (WIN_R * WIN_C, rows * span), 0)
    place = lax.broadcasted_iota(jnp.int32, (WIN_R * WIN_C, rows * span), 1)
    row_slot = (place % rows - place // span + HALF_R) % rows
    col_slot = (place % span) // rows
    pick = (slot // WIN_C == row_slot) & (slot % WIN_C == col_slot)
    flat = rel_bias.reshape(layers * heads, WIN_R * WIN_C) * LOG2E
    base = jnp.dot(flat, pick.astype(F32), precision=lax.Precision.HIGHEST)
    base = jnp.where(row_slot[:1] < WIN_R, base, MASKED)
    base = base.reshape(layers * heads, rows, span)
    return jnp.pad(base, ((0, 0), (0, 0), (0, window - span)), constant_values=MASKED)


def body(token_grid, norm_gain, w_query, w_key, w_value, w_out, rel_bias, *, order):
    n_sp = lax.axis_size("sp")
    n_tp = lax.axis_size("tp")
    n_y = n_tp // 2
    layers = norm_gain.shape[0]
    chunk = token_grid.shape[1]
    columns = token_grid.shape[2]
    rows = n_sp * token_grid.shape[0]
    cols = columns // n_sp
    tokens = rows * cols
    halo = HALF_C * rows
    window = BLOCK + 2 * halo
    here = lax.axis_index("tp").astype(jnp.int32)
    my_y, my_core = here // 2, here % 2
    rank = [order.index(i) for i in range(n_sp)]
    after_of = [(order[i], order[(i + 1) % n_sp]) for i in range(n_sp)]
    before_of = [(b, a) for a, b in after_of]

    if tokens == 4 * BLOCK and halo <= BLOCK and BLOCK % rows == 0:
        per = BLOCK // rows
        parts = [
            (list(range(per, 3 * per)), [BLOCK, 2 * BLOCK]),
            (list(range(per)) + list(range(3 * per, 4 * per)), [0, 3 * BLOCK]),
        ]
    else:
        parts = [(list(range(cols)), list(range(0, tokens, BLOCK)))]
    count = len(parts)

    def over_core(x):
        return lax.ppermute(x, "tp", [(i, i ^ 1) for i in range(n_tp)])

    def over_y(x, shift):
        return lax.ppermute(x, "tp", [(i, (i + 2 * shift) % n_tp) for i in range(n_tp)])

    picks = [(cols_of, rank) for cols_of, _ in parts]
    sends = split_columns(token_grid[0], picks, n_sp)
    mine = []
    for send in sends:
        got = lax.all_to_all(send, "sp", 0, 0, tiled=True)
        mine.append(to_column_order(got))

    theirs = [
        lax.dynamic_slice_in_dim(w_out, (2 * y + 1 - my_core) * chunk, chunk, 2)
        for y in range(n_y)
    ]
    w_other = over_core(jnp.stack(theirs))
    gains = norm_gain.astype(F32).reshape(layers, n_tp, 1, chunk)
    bias = expand_bias(dense_bias(rel_bias, rows, window), rows)

    behind = [(my_y - shift) % n_y for shift in range(n_y)]
    ahead = [(my_y + shift) % n_y for shift in range(n_y)]
    every = [jnp.int32(y) for y in range(n_y)]

    def chunk_ids(ys):
        return jnp.stack([2 * y + my_core for y in ys] + [2 * y + 1 - my_core for y in ys])

    grids = [[x] + [over_y(x, shift) for shift in range(1, n_y)] for x in mine]
    for layer in range(layers):
        ids = chunk_ids(behind if layer == 0 else every)
        made = []
        for at, grid in enumerate(grids):
            made.append(
                qkv(
                    layer,
                    grid + [over_core(x) for x in grid],
                    ids,
                    gains,
                    w_query,
                    w_key,
                    w_value,
                    halo if at == count - 1 else 0,
                )
            )
        first, last = made[-1][3:]
        after = lax.ppermute(first, "sp", before_of)
        before = lax.ppermute(last, "sp", after_of)
        own_kv = [array for one in made for array in one[1:3]]
        segments = []
        for at, (_, starts) in enumerate(parts):
            for i, start in enumerate(starts):
                segments.append((start, BLOCK, (2 * at, 2 * at + 1), i * BLOCK))
        ends = [
            (-halo, halo, 2 * count, 0),
            (tokens, halo, 2 * count + 1, 0),
        ]
        fresh = []
        for at, (cols_of, starts) in enumerate(parts):
            last_part = at == count - 1
            mixed = attention(
                layer,
                starts,
                made[at][0],
                own_kv + ([before, after] if last_part else []),
                sorted(segments + (ends if last_part else [])),
                bias,
            )
            mixed_other = over_core(mixed)
            if layer + 1 < layers:
                partial = project(
                    layer, mixed, mixed_other, w_out, w_other, jnp.stack(every), my_core, True
                )[0]
                partials = [partial] + [over_y(partial, shift) for shift in range(1, n_y)]
                if layer == 0:
                    where = jnp.stack([(my_y - y) % n_y for y in every])
                else:
                    where = jnp.zeros((n_y,), jnp.int32)
                fresh.append([add_update(grids[at], partials, where)])
            else:
                ys = jnp.stack(ahead[1:] + ahead[:1])
                made_of = project(layer, mixed, mixed_other, w_out, w_other, ys, my_core, False)
                partials = [made_of[-1]]
                partials += [over_y(made_of[shift - 1], shift) for shift in range(1, n_y)]
                done = finish(grids[at][0], partials, my_y, rows, len(cols_of))
                fresh.append(lax.all_to_all(done, "sp", 0, 0, tiled=True))
        grids = fresh

    return merge_columns(grids, picks, columns, n_sp)[None]


def solution(mesh):
    in_specs = (
        P("sp", "tp", None),
        P(),
        P(None, None, "tp"),
        P(None, None, "tp"),
        P(None, None, "tp"),
        P(None, "tp", None),
        P(None, "tp", None, None),
    )
    out_specs = P("sp", "tp", None)
    return jax.shard_map(
        functools.partial(body, order=ring_order(mesh)),
        mesh=mesh,
        in_specs=in_specs,
        out_specs=out_specs,
        check_vma=False,
    )
```
